32 devices in a mesh: fs: 8 (over z, y), tp: 4 (over x, core).
Axes of the slice: x: 2, y: 2, z: 4, core: 2. Of those that a mesh axis runs over, the one named last changes fastest.
Arguments:
- saved_input: bfloat16 [6144, 2048], P('fs'), may hold values from -6 to 6
- cot_inproj: bfloat16 [6144, 1024], P('fs', 'tp'), may hold values from -0.076171875 to 0.076171875
- cot_outproj: bfloat16 [6144, 1024], P('fs', 'tp'), may hold values from -0.076171875 to 0.076171875
- factor_inproj: bfloat16 [2048, 256], P('fs')
- factor_outproj: bfloat16 [2048, 256], P('fs')
- weight_inproj: float32 [2048, 1024], P('fs', 'tp'), may hold values from -0.125 to 0.125
- weight_outproj: float32 [2048, 1024], P('fs', 'tp'), may hold values from -0.125 to 0.125
- first_inproj: float32 [256, 1024], P('fs', 'tp'), may hold values from -6 to 6
- first_outproj: float32 [256, 1024], P('fs', 'tp'), may hold values from -6 to 6
- second_inproj: float32 [256, 1024], P('fs', 'tp'), may hold values from 0.25 to 4
- second_outproj: float32 [256, 1024], P('fs', 'tp'), may hold values from 0.25 to 4
Outputs:
- update_inproj: float32 [2048, 1024], P('fs', 'tp')
- update_outproj: float32 [2048, 1024], P('fs', 'tp')
- new_inproj: float32 [2048, 1024], P('fs', 'tp')
- new_outproj: float32 [2048, 1024], P('fs', 'tp')
- copy_inproj: bfloat16 [2048, 1024], P(None, 'tp')
- copy_outproj: bfloat16 [2048, 1024], P(None, 'tp')
- first_inproj_new: float32 [256, 1024], P('fs', 'tp')
- first_outproj_new: float32 [256, 1024], P('fs', 'tp')
- second_inproj_new: float32 [256, 1024], P('fs', 'tp')
- second_outproj_new: float32 [256, 1024], P('fs', 'tp')
The draws below stay inside these ranges and needn't reach their ends.
All inputs are finite; a program needn't handle non-finite values.
Results may differ from the reference program's by a relative error of at most 0.00045.
Values may be sent and summed in bfloat16 or wider, within the bound.
No kernel may reach another device: no remote copies, remote signals or barrier semaphores. Data moves between devices by JAX's collectives and lax.ppermute only.
A program may use at most 64 MiB of HBM per device.

```python
import math
import jax
import jax.numpy as jnp
from jax import lax

D = 2048
RANK = 256
GN = 1024
TOKENS = 6144


def lowrank_draw(key):
    base = jax.random.normal(key, (D, RANK), jnp.float32)
    position = jnp.arange(D).astype(jnp.float32) / D
    scale = jnp.exp(jnp.log(10.0) * position) * 0.22 * D ** (-0.5)
    return (base * scale[:, None]).astype(jnp.bfloat16)


def draw_factor_inproj(key, part):
    return lowrank_draw(jax.random.fold_in(key, 11))


def draw_factor_outproj(key, part):
    return lowrank_draw(jax.random.fold_in(key, 12))


def raised(values, stream_key, source, target, shards_of, factor):
    owner, partner = [(jnp.arange(values.shape[dim]) // (values.shape[dim] // shards_of)).reshape([-1 if axis == dim else 1 for axis in range(values.ndim)]) for dim in (source, target)]
    chosen = jax.random.permutation(stream_key, shards_of)[partner]
    strong = (owner == chosen) | (owner == (partner + shards_of // 2) % shards_of)
    return jnp.where(strong, factor * values, values)


def levels(rng, shape, cuts, least, high):
    level = 1.0
    for axis_at, shards_of in cuts:
        draws = jax.random.uniform(jax.random.fold_in(jax.random.fold_in(rng, 6), axis_at), (shards_of,), jnp.float32, least / len(cuts), high / len(cuts))
        level = level * jnp.repeat(jnp.exp(draws), shape[axis_at] // shards_of).reshape((-1,) + (1,) * (len(shape) - 1 - axis_at))
    return level


def normal_values(key, dims, spread, most, cuts=(), kind=jnp.bfloat16):
    array = spread * jax.random.normal(key, dims, jnp.float32)
    if cuts:
        array = array * levels(key, dims, cuts, -0.22, 0.18)
    return jnp.clip(array, -most, most).astype(kind)


def gaussian_with(stream_key, shape, width, limit, split, heavy, kind=jnp.bfloat16):
    array = width * jax.random.normal(stream_key, shape, jnp.float32)
    if split:
        array = array * levels(stream_key, shape, split, -0.22, 0.18)
    return jnp.clip(raised(array, jax.random.fold_in(stream_key, 3), *heavy), -limit, limit).astype(kind)


def setup_inputs(seed: int = 0) -> dict:
    streams_of = jax.random.split(jax.random.key(seed), 12)
    saved_input = gaussian_with(streams_of[0], (TOKENS, D), 1.0, 6.0, ((0, 8),), (0, 1, 8, 2.0))
    cot_inproj = normal_values(streams_of[1], (TOKENS, GN), (TOKENS ** -0.5), 0.076171875, ((0, 8), (1, 4)))
    cot_outproj = normal_values(streams_of[2], (TOKENS, GN), (TOKENS ** -0.5), 0.076171875, ((0, 8), (1, 4)))
    factor_inproj = draw_factor_inproj(jax.random.fold_in(streams_of[11], 71), 0)
    factor_outproj = draw_factor_outproj(jax.random.fold_in(streams_of[11], 71), 0)
    weight_inproj = normal_values(streams_of[5], (D, GN), D ** -0.5, 0.125, ((0, 8), (1, 4)), jnp.float32)
    weight_outproj = normal_values(streams_of[6], (D, GN), D ** -0.5, 0.125, ((0, 8), (1, 4)), jnp.float32)
    first_inproj = normal_values(streams_of[7], (RANK, GN), 1.0, 6.0, ((0, 8), (1, 4)), jnp.float32)
    first_outproj = normal_values(streams_of[8], (RANK, GN), 1.0, 6.0, ((0, 8), (1, 4)), jnp.float32)
    second_inproj = jnp.clip(jnp.exp(math.log(4.0) - 2.7725887 * jax.random.uniform(streams_of[9], (RANK, GN), jnp.float32) ** levels(streams_of[9], (RANK, GN), ((0, 8), (1, 4)), -0.2, 0.2)), 0.25, 4.0)
    second_outproj = jnp.clip(jnp.exp(math.log(4.0) - 2.7725887 * jax.random.uniform(streams_of[10], (RANK, GN), jnp.float32) ** levels(streams_of[10], (RANK, GN), ((0, 8), (1, 4)), -0.2, 0.2)), 0.25, 4.0)
    return dict(saved_input=saved_input, cot_inproj=cot_inproj, cot_outproj=cot_outproj, factor_inproj=factor_inproj, factor_outproj=factor_outproj, weight_inproj=weight_inproj, weight_outproj=weight_outproj, first_inproj=first_inproj, first_outproj=first_outproj, second_inproj=second_inproj, second_outproj=second_outproj)


def one_matrix(saved_input, cotangent, factor, weight, first, second):
    grad = lax.dot_general(saved_input, cotangent, (((0,), (0,)), ((), ())), preferred_element_type=jnp.float32)
    factor_wide = factor.astype(jnp.float32)
    projected = lax.dot_general(factor_wide, grad, (((0,), (0,)), ((), ())), precision=lax.Precision.HIGHEST)
    first_new = 0.8 * first + 0.2 * projected
    second_new = 0.9 * second + 0.1 * projected * projected
    small = first_new / (jnp.sqrt(second_new) + 1e-08)
    full = jnp.dot(factor_wide, small, precision=lax.Precision.HIGHEST)
    update = full / jnp.sqrt(jnp.mean(full * full) + 1e-06)
    fresh = weight - 0.02 * update
    return (update, fresh, fresh.astype(jnp.bfloat16), first_new, second_new)

def reference(saved_input, cot_inproj, cot_outproj, factor_inproj, factor_outproj, weight_inproj, weight_outproj, first_inproj, first_outproj, second_inproj, second_outproj):
    in_parts = one_matrix(saved_input, cot_inproj, factor_inproj, weight_inproj, first_inproj, second_inproj)
    out_parts = one_matrix(saved_input, cot_outproj, factor_outproj, weight_outproj, first_outproj, second_outproj)
    return (in_parts[0], out_parts[0], in_parts[1], out_parts[1], in_parts[2], out_parts[2], in_parts[3], out_parts[3], in_parts[4], out_parts[4])
```

```python
import jax
import jax.numpy as jnp
from jax import lax
from jax.sharding import PartitionSpec as P

HIGHEST = lax.Precision.HIGHEST


def flip(x, axis, bit):
    size = lax.axis_size(axis)
    return lax.ppermute(x, axis, [(i, i ^ bit) for i in range(size)])


def gather_blocks(x):
    size = lax.axis_size("fs")
    if size != 8:
        everyone = lax.all_gather(x, "fs", axis=0, tiled=False)
        here = lax.axis_index("fs")
        return [
            (d, lax.dynamic_index_in_dim(everyone, here ^ d, 0, keepdims=False)) for d in range(size)
        ]
    far, middle, near = flip(x, "fs", 6), flip(x, "fs", 4), flip(x, "fs", 2)
    side = flip(x, "fs", 1)
    return [
        (0, x),
        (1, side),
        (2, near),
        (3, flip(near, "fs", 1)),
        (4, middle),
        (5, flip(middle, "fs", 1)),
        (6, far),
        (7, flip(far, "fs", 1)),
    ]


def in_order(blocks):
    here = lax.axis_index("fs")
    rows = blocks[0][1].shape[0]
    whole = jnp.zeros((rows * len(blocks),) + blocks[0][1].shape[1:], blocks[0][1].dtype)
    for d, block in blocks:
        whole = lax.dynamic_update_slice_in_dim(whole, block, (here ^ d) * rows, 0)
    return whole


def sum_scatter(x):
    size = lax.axis_size("fs")
    if size != 8:
        return lax.psum_scatter(x, "fs", scatter_dimension=0, tiled=True)
    here = lax.axis_index("fs")
    rows = x.shape[0] // size
    total = lax.dynamic_slice_in_dim(x, here * rows, rows, 0)
    for d in (7, 6, 5, 4, 3, 2, 1):
        total = total + flip(lax.dynamic_slice_in_dim(x, (here ^ d) * rows, rows, 0), "fs", d)
    return total


def on_device(
    saved_input,
    cot_inproj,
    cot_outproj,
    factor_inproj,
    factor_outproj,
    weight_inproj,
    weight_outproj,
    first_inproj,
    first_outproj,
    second_inproj,
    second_outproj,
):
    odd = lax.axis_index("tp") % 2 == 1

    def mine(a, b):
        return jnp.where(odd, b, a)

    def theirs(a, b):
        return jnp.where(odd, a, b)

    factor = mine(factor_inproj, factor_outproj)
    factors = in_order(gather_blocks(factor))
    cot = mine(cot_inproj, cot_outproj)
    cot_peer = flip(theirs(cot_inproj, cot_outproj), "tp", 1)
    moments = jnp.stack([mine(first_inproj, first_outproj), mine(second_inproj, second_outproj)])
    moments_peer = flip(
        jnp.stack([theirs(first_inproj, first_outproj), theirs(second_inproj, second_outproj)]), "tp", 1
    )
    mapped = jnp.dot(saved_input, factors, preferred_element_type=jnp.float32)
    both = jnp.concatenate([cot, cot_peer], axis=1).astype(jnp.float32)
    term = lax.dot_general(
        mapped, both, (((0,), (0,)), ((), ())), precision=HIGHEST, preferred_element_type=jnp.float32
    )
    square = lax.dot_general(
        factors, factors, (((0,), (0,)), ((), ())), preferred_element_type=jnp.float32
    )
    projected = sum_scatter(term)
    first = jnp.concatenate([moments[0], moments_peer[0]], axis=1)
    second = jnp.concatenate([moments[1], moments_peer[1]], axis=1)
    first_new = 0.8 * first + 0.2 * projected
    second_new = 0.9 * second + 0.1 * projected * projected
    small = first_new / (jnp.sqrt(second_new) + 1e-08)
    columns = cot.shape[1]
    moments_new = jnp.stack([first_new[:, :columns], second_new[:, :columns]])
    moments_other = flip(jnp.stack([first_new[:, columns:], second_new[:, columns:]]), "tp", 1)
    smalls = in_order(gather_blocks(small))
    full = jnp.dot(factor.astype(jnp.float32), smalls, precision=HIGHEST)
    total = jnp.sum(smalls * jnp.dot(square, smalls, precision=HIGHEST))
    full_other = flip(full[:, columns:], "tp", 1)
    full_mine = full[:, :columns]
    total = jnp.full((8, 128), total, jnp.float32)
    bit = 2
    while bit < lax.axis_size("tp"):
        total = total + flip(total, "tp", bit)
        bit *= 2
    total_other = flip(total, "tp", 1)
    entries = float(full.shape[0] * columns * lax.axis_size("fs") * lax.axis_size("tp"))
    norm_mine = jnp.sqrt(jnp.maximum(total[0, 0], 0.0) / entries + 1e-06)
    norm_other = jnp.sqrt(jnp.maximum(total_other[0, 0], 0.0) / entries + 1e-06)
    update_mine = full_mine / norm_mine
    update_other = full_other / norm_other
    update_in, update_out = mine(update_mine, update_other), mine(update_other, update_mine)
    fresh_in = weight_inproj - 0.02 * update_in
    fresh_out = weight_outproj - 0.02 * update_out
    copies = gather_blocks(jnp.stack([fresh_in.astype(jnp.bfloat16), fresh_out.astype(jnp.bfloat16)]))
    copy_in = in_order([(d, block[0]) for d, block in copies])
    copy_out = in_order([(d, block[1]) for d, block in copies])
    return (
        update_in,
        update_out,
        fresh_in,
        fresh_out,
        copy_in,
        copy_out,
        mine(moments_new[0], moments_other[0]),
        mine(moments_other[0], moments_new[0]),
        mine(moments_new[1], moments_other[1]),
        mine(moments_other[1], moments_new[1]),
    )


def solution(mesh):
    rows, split = P("fs", None), P("fs", "tp")
    return jax.shard_map(
        on_device,
        mesh=mesh,
        in_specs=(rows, split, split, rows, rows) + (split,) * 6,
        out_specs=(split,) * 4 + (P(None, "tp"),) * 2 + (split,) * 4,
        check_vma=False,
    )
```

```python
import functools

import jax
import jax.numpy as jnp
from jax import lax
from jax.experimental import pallas as pl
from jax.experimental.pallas import tpu as pltpu
from jax.sharding import PartitionSpec as P

HIGHEST = lax.Precision.HIGHEST
VMEM = pl.BlockSpec(memory_space=pltpu.VMEM)
SMEM = pl.BlockSpec(memory_space=pltpu.SMEM)
VMEM_BYTES = 16 * 2**20
ROWS = (((0,), (0,)), ((), ()))


def flip(x, axis, bit):
    size = lax.axis_size(axis)
    return lax.ppermute(x, axis, [(i, i ^ bit) for i in range(size)])


def pairwise():
    return lax.axis_size("fs") == 8


def gather_blocks(x):
    size = lax.axis_size("fs")
    if not pairwise():
        everyone = lax.all_gather(x, "fs", axis=0, tiled=False)
        here = lax.axis_index("fs")
        return [
            lax.dynamic_index_in_dim(everyone, here ^ d, 0, keepdims=False) for d in range(size)
        ]
    far, middle, near = flip(x, "fs", 6), flip(x, "fs", 4), flip(x, "fs", 2)
    side = flip(x, "fs", 1)
    return [
        x,
        side,
        near,
        flip(near, "fs", 1),
        middle,
        flip(middle, "fs", 1),
        far,
        flip(far, "fs", 1),
    ]


def in_order(blocks):
    here = lax.axis_index("fs")
    rows = blocks[0].shape[0]
    whole = jnp.zeros((rows * len(blocks),) + blocks[0].shape[1:], blocks[0].dtype)
    for d, block in enumerate(blocks):
        whole = lax.dynamic_update_slice_in_dim(whole, block, (here ^ d) * rows, 0)
    return whole


def thirds(x):
    high = x.astype(jnp.bfloat16)
    rest = x - high.astype(jnp.float32)
    middle = rest.astype(jnp.bfloat16)
    low = (rest - middle.astype(jnp.float32)).astype(jnp.bfloat16)
    return high, middle, low


def call(body, outs, *args, scratch=(), flops):
    size = sum(a.size * a.dtype.itemsize for a in args)
    return pl.pallas_call(
        body,
        out_shape=outs,
        in_specs=[SMEM if a.dtype == jnp.int32 else VMEM for a in args],
        out_specs=jax.tree.map(lambda _: VMEM, outs),
        scratch_shapes=list(scratch),
        compiler_params=pltpu.CompilerParams(vmem_limit_bytes=VMEM_BYTES),
        cost_estimate=pl.CostEstimate(flops=flops, bytes_accessed=size, transcendentals=0),
    )(*args)


def map_body(size, here_ref, saved_ref, *refs):
    factors, (cot_ref, peer_ref, term_ref) = refs[:size], refs[size:]
    here = here_ref[0]
    depth, rank = factors[0].shape
    mapped = jnp.zeros((saved_ref.shape[0], rank), jnp.float32)
    for d, factor in enumerate(factors):
        at = pl.multiple_of((here ^ d) * depth, depth)
        mapped += jnp.dot(
            saved_ref[:, pl.ds(at, depth)], factor[...], preferred_element_type=jnp.float32
        )
    parts = thirds(mapped)
    columns = cot_ref.shape[1]
    rows = rank // size
    for side, cot in enumerate((cot_ref, peer_ref)):
        term = sum(
            lax.dot_general(part, cot[...], ROWS, preferred_element_type=jnp.float32)
            for part in parts[::-1]
        )
        for k in range(size):
            term_ref[here ^ k, :, side * columns : (side + 1) * columns] = term[
                k * rows : (k + 1) * rows, :
            ]


def square_body(*refs):
    total = jnp.zeros(refs[-1].shape, jnp.float32)
    for factor in refs[:-1]:
        total += lax.dot_general(factor[...], factor[...], ROWS, preferred_element_type=jnp.float32)
    refs[-1][...] = total


def full_body(size, here_ref, factor_ref, square_ref, *refs):
    smalls, (full_ref, other_ref, sum_ref, held) = refs[:size], refs[size:]
    rows = smalls[0].shape[0]
    for d, small in enumerate(smalls):
        at = pl.multiple_of((here_ref[0] ^ d) * rows, rows)
        held[pl.ds(at, rows), :] = small[...]
    columns = full_ref.shape[1]
    small = held[...]
    full = sum(
        jnp.dot(factor_ref[...], part, preferred_element_type=jnp.float32)
        for part in thirds(small)[::-1]
    )
    full_ref[...] = full[:, :columns]
    other_ref[...] = full[:, columns:]
    product = small * jnp.dot(square_ref[...], small, precision=HIGHEST)
    sum_ref[...] = jnp.full(sum_ref.shape, jnp.sum(product), jnp.float32)


def finish_body(entries, odd_ref, sums_ref, others_ref, full_ref, other_ref, *refs):
    weights, (up_in, up_out, new_in, new_out, copy) = refs[:2], refs[2:]
    odd = odd_ref[0] == 1

    def norm(ref):
        mean = jnp.maximum(jnp.sum(ref[...], axis=0), 0.0) / entries
        return jnp.sqrt(mean + 1e-06)[0:1, 0:1]

    update = full_ref[...] / norm(sums_ref)
    update_other = other_ref[...] / norm(others_ref)
    for k, (up, new, weight) in enumerate(
        ((up_in, new_in, weights[0]), (up_out, new_out, weights[1]))
    ):
        chosen = jnp.where(odd, update, update_other) if k else jnp.where(odd, update_other, update)
        up[...] = chosen
        fresh = weight[...] - 0.02 * chosen
        new[...] = fresh
        copy[k] = fresh.astype(jnp.bfloat16)


def on_device(
    saved_input,
    cot_inproj,
    cot_outproj,
    factor_inproj,
    factor_outproj,
    weight_inproj,
    weight_outproj,
    first_inproj,
    first_outproj,
    second_inproj,
    second_outproj,
):
    odd = lax.axis_index("tp") % 2 == 1
    size, split = lax.axis_size("fs"), lax.axis_size("tp")
    here = lax.axis_index("fs").astype(jnp.int32).reshape(1)
    f32 = functools.partial(jax.ShapeDtypeStruct, dtype=jnp.float32)

    def mine(a, b):
        return jnp.where(odd, b, a)

    def theirs(a, b):
        return jnp.where(odd, a, b)

    factor = mine(factor_inproj, factor_outproj)
    depth, rank = factor.shape
    columns = cot_inproj.shape[1]
    factors = gather_blocks(factor)
    cot = mine(cot_inproj, cot_outproj)
    cot_peer = flip(theirs(cot_inproj, cot_outproj), "tp", 1)
    moments = jnp.stack([mine(first_inproj, first_outproj), mine(second_inproj, second_outproj)])
    moments_peer = flip(
        jnp.stack([theirs(first_inproj, first_outproj), theirs(second_inproj, second_outproj)]), "tp", 1
    )
    if pairwise():
        tokens = saved_input.shape[0]
        term = call(
            functools.partial(map_body, size),
            f32((size, rank // size, 2 * columns)),
            here,
            saved_input,
            *factors,
            cot,
            cot_peer,
            flops=2 * tokens * rank * (depth * size + 6 * columns),
        )
        square = call(square_body, f32((rank, rank)), *factors, flops=2 * rank * rank * depth * size)
        projected = term[0] + sum(flip(term[d], "fs", d) for d in (7, 6, 5, 4, 3, 2, 1))
    else:
        factors = in_order(factors)
        mapped = jnp.dot(saved_input, factors, preferred_element_type=jnp.float32)
        both = jnp.concatenate([cot, cot_peer], axis=1).astype(jnp.float32)
        term = lax.dot_general(mapped, both, ROWS, precision=HIGHEST)
        square = lax.dot_general(factors, factors, ROWS, preferred_element_type=jnp.float32)
        projected = lax.psum_scatter(term, "fs", scatter_dimension=0, tiled=True)
    first = jnp.concatenate([moments[0], moments_peer[0]], axis=1)
    second = jnp.concatenate([moments[1], moments_peer[1]], axis=1)
    first_new = 0.8 * first + 0.2 * projected
    second_new = 0.9 * second + 0.1 * projected * projected
    small = first_new / (jnp.sqrt(second_new) + 1e-08)
    moments_new = jnp.stack([first_new[:, :columns], second_new[:, :columns]])
    moments_other = flip(jnp.stack([first_new[:, columns:], second_new[:, columns:]]), "tp", 1)
    smalls = gather_blocks(small)
    if pairwise():
        full, full_other, total = call(
            functools.partial(full_body, size),
            (f32((depth, columns)), f32((depth, columns)), f32((8, 128))),
            here,
            factor,
            square,
            *smalls,
            scratch=[pltpu.VMEM((rank, 2 * columns), jnp.float32)],
            flops=2 * rank * 2 * columns * (3 * depth + 6 * rank),
        )
    else:
        smalls = in_order(smalls)
        full = jnp.dot(factor.astype(jnp.float32), smalls, precision=HIGHEST)
        total = jnp.sum(smalls * jnp.dot(square, smalls, precision=HIGHEST))
        total = jnp.full((8, 128), total, jnp.float32)
        full, full_other = full[:, :columns], full[:, columns:]
    full_other = flip(full_other, "tp", 1)
    totals = [total] + [flip(total, "tp", k) for k in range(1, split)]
    sums, sums_other = jnp.stack(totals[0::2]), jnp.stack(totals[1::2])
    entries = float(depth * size * columns * split)
    shard = f32((depth, columns))
    update_in, update_out, fresh_in, fresh_out, copies = call(
        functools.partial(finish_body, entries),
        (shard,) * 4 + (jax.ShapeDtypeStruct((2, depth, columns), jnp.bfloat16),),
        odd.astype(jnp.int32).reshape(1),
        sums,
        sums_other,
        full,
        full_other,
        weight_inproj,
        weight_outproj,
        flops=10 * depth * columns,
    )
    copies = gather_blocks(copies)
    copy_in = in_order([block[0] for block in copies])
    copy_out = in_order([block[1] for block in copies])
    return (
        update_in,
        update_out,
        fresh_in,
        fresh_out,
        copy_in,
        copy_out,
        mine(moments_new[0], moments_other[0]),
        mine(moments_other[0], moments_new[0]),
        mine(moments_new[1], moments_other[1]),
        mine(moments_other[1], moments_new[1]),
    )


def solution(mesh):
    rows, split = P("fs", None), P("fs", "tp")
    return jax.shard_map(
        on_device,
        mesh=mesh,
        in_specs=(rows, split, split, rows, rows) + (split,) * 6,
        out_specs=(split,) * 4 + (P(None, "tp"),) * 2 + (split,) * 4,
        check_vma=False,
    )
```

```python
import functools

import jax
import jax.numpy as jnp
from jax import lax
from jax.experimental import pallas as pl
from jax.experimental.pallas import tpu as pltpu
from jax.sharding import PartitionSpec as P

HIGHEST = lax.Precision.HIGHEST
VMEM = pl.BlockSpec(memory_space=pltpu.VMEM)
HBM = pl.BlockSpec(memory_space=pltpu.HBM)
VMEM_BYTES = 16 * 2**20
ROWS = (((0,), (0,)), ((), ()))


def send(x, axis, bit):
    size = lax.axis_size(axis)
    return lax.ppermute(x, axis, [(i, i ^ bit) for i in range(size)])


def thirds(x):
    high = x.astype(jnp.bfloat16)
    rest = x - high.astype(jnp.float32)
    middle = rest.astype(jnp.bfloat16)
    low = (rest - middle.astype(jnp.float32)).astype(jnp.bfloat16)
    return high, middle, low


def exact_dot(left, right, dims=(((1,), (0,)), ((), ()))):
    wide = left.dtype == jnp.float32
    total = None
    for part in thirds(left if wide else right)[::-1]:
        pair = (part, right) if wide else (left, part)
        term = lax.dot_general(*pair, dims, preferred_element_type=jnp.float32)
        total = term if total is None else total + term
    return total


def call(body, outs, *args, scratch=(), flops, hbm=(), out=VMEM, aliases={}):
    size = sum(a.size * a.dtype.itemsize for a in args)
    args = [
        pltpu.with_memory_space_constraint(a, pltpu.HBM) if k in hbm else a
        for k, a in enumerate(args)
    ]
    return pl.pallas_call(
        body,
        out_shape=outs,
        in_specs=[HBM if k in hbm else VMEM for k in range(len(args))],
        out_specs=jax.tree.map(lambda _: out, outs),
        scratch_shapes=list(scratch),
        input_output_aliases=aliases,
        compiler_params=pltpu.CompilerParams(vmem_limit_bytes=VMEM_BYTES),
        cost_estimate=pl.CostEstimate(flops=flops, bytes_accessed=size, transcendentals=0),
    )(*args)


def is_odd():
    return lax.axis_index("tp") % 2 == 1


def slot(d, rows):
    return pl.ds(pl.multiple_of((lax.axis_index("fs") ^ d) * rows, rows), rows)


def copy_all(copies):
    for copy in copies:
        copy.start()
    for copy in copies:
        copy.wait()


def pick_body(even, odd, out, sem):
    @pl.when(is_odd())
    def _():
        copy_all([pltpu.make_async_copy(odd, out, sem)])

    @pl.when(jnp.logical_not(is_odd()))
    def _():
        copy_all([pltpu.make_async_copy(even, out, sem)])


def picked_body(cots, firsts, seconds, factors, weights, cot, moments, factor, both, w4a, w4b, sems):
    depth = factor.shape[0]
    half = w4b.shape[0]

    def copies(k):
        pairs = (
            (cots[k], cot),
            (firsts[k], moments.at[0]),
            (seconds[k], moments.at[1]),
            (factors[k], factor),
            (weights[0], both.at[0]),
            (weights[1], both.at[1]),
            (weights[0], w4a.at[pl.ds(0, depth), :]),
            (weights[1].at[pl.ds(0, depth - half), :], w4a.at[pl.ds(depth, depth - half), :]),
            (weights[1].at[pl.ds(depth - half, half), :], w4b),
        )
        return [pltpu.make_async_copy(*pair, sems.at[i]) for i, pair in enumerate(pairs)]

    @pl.when(is_odd())
    def _():
        copy_all(copies(0))

    @pl.when(jnp.logical_not(is_odd()))
    def _():
        copy_all(copies(1))


def fetch(saved_ref, held, sems, numbers):
    copies = [
        pltpu.make_async_copy(saved_ref.at[:, slot(d, held.shape[2])], held.at[k], sems.at[k])
        for k, d in enumerate(numbers)
    ]
    for copy in copies:
        copy.start()
    return copies


def add_blocks(total, copies, held, factors):
    for k, (copy, factor) in enumerate(zip(copies, factors, strict=True)):
        copy.wait()
        total = total + jnp.dot(held[k], factor[...], preferred_element_type=jnp.float32)
    return total


def map_body(numbers, saved_ref, *refs):
    factors, (mapped_ref, held, sems) = refs[:-3], refs[-3:]
    copies = fetch(saved_ref, held, sems, numbers)
    mapped_ref[...] = add_blocks(jnp.zeros(mapped_ref.shape, jnp.float32), copies, held, factors)


def term_body(size, numbers, saved_ref, mapped_ref, *refs):
    factors, refs = refs[: len(numbers)], refs[len(numbers) :]
    cot_in, cot_out, peer, far, near, own, held, cot, sems, cot_sem = refs
    copies = fetch(saved_ref, held, sems, numbers)

    @pl.when(is_odd())
    def _():
        pltpu.make_async_copy(cot_out, cot, cot_sem).start()

    @pl.when(jnp.logical_not(is_odd()))
    def _():
        pltpu.make_async_copy(cot_in, cot, cot_sem).start()

    mapped = add_blocks(mapped_ref[...], copies, held, factors)
    columns = cot.shape[1]
    rows = mapped.shape[1] // size
    here = lax.axis_index("fs")
    pltpu.make_async_copy(cot_in, cot, cot_sem).wait()
    for side, right in enumerate((cot, peer)):
        term = exact_dot(mapped, right[...], ROWS)
        at = slice(side * columns, (side + 1) * columns)
        for k in range(size):
            own[here ^ k, :, at] = term[k * rows : (k + 1) * rows, :]
    for ref, first in ((far, 7), (near, 3)):
        ref[0] = own[first]
        ref[1] = own[first - 2]


def add_body(own, far, a4, a6):
    a4[...] = own[4] + far[1]
    a6[...] = own[6] + far[0]


def add_near_body(own, near, a2):
    a2[...] = own[2] + near[0]


def moments_body(own, near, r4, r6, r2, f_in, f_out, s_in, s_out, peer, small, mine, other):
    odd = is_odd()
    projected = own[0] + near[1] + r4[...] + r6[...] + r2[...]
    columns = f_in.shape[1]
    pairs = (
        (jnp.where(odd, f_out[...], f_in[...]), jnp.where(odd, s_out[...], s_in[...]), mine),
        (peer[0], peer[1], other),
    )
    for side, (first, second, new) in enumerate(pairs):
        at = slice(side * columns, (side + 1) * columns)
        x = projected[:, at]
        first_new = 0.8 * first + 0.2 * x
        second_new = 0.9 * second + 0.1 * x * x
        new[0] = first_new
        new[1] = second_new
        small[:, at] = first_new / (jnp.sqrt(second_new) + 1e-08)


def square_body(size, *refs):
    factors, (square_ref, held) = refs[:size], refs[size:]
    for d, factor in enumerate(factors):
        held[slot(d, factor.shape[0]), :] = factor[...]
    square_ref[...] = lax.dot_general(
        held[...], held[...], ROWS, preferred_element_type=jnp.float32
    )


def sum_body(size, square_ref, *refs):
    smalls, (sum_ref, mine_ref, other_ref) = refs[:size], refs[size:]
    columns = mine_ref.shape[1]
    for d, small in enumerate(smalls):
        at = slot(d, small.shape[0])
        mine_ref[at, :] = small[:, :columns]
        other_ref[at, :] = small[:, columns:]
    product = sum(
        ref[...] * jnp.dot(square_ref[...], ref[...], precision=HIGHEST)
        for ref in (mine_ref, other_ref)
    )
    sum_ref[...] = jnp.full(sum_ref.shape, jnp.sum(product), jnp.float32)


def full_body(small_ref, *refs):
    small, full_ref = thirds(small_ref[...])[::-1], refs[-1]
    for k, factor in enumerate(refs[:-1]):
        full_ref[k] = sum(
            jnp.dot(factor[...], part, preferred_element_type=jnp.float32) for part in small
        )


def finish_body(entries, sums, full_ref, other_ref, weights, news, back, outs):
    odd = is_odd()
    up_in, up_out, new_in, new_out, copies, firsts, seconds = outs

    def scale(pair):
        mean = jnp.maximum(pair[0][...] + pair[1][...], 0.0) / entries
        return (1.0 / jnp.sqrt(mean + 1e-06))[0:1, 0:1]

    scales = scale(sums[:2]), scale(sums[2:])
    for k, (copy, both) in enumerate(zip(copies, weights, strict=True)):
        update = full_ref[k] * scales[0]
        update_other = other_ref[k] * scales[1]
        for p, weight in enumerate(both):
            chosen = jnp.where(odd, update, update_other) if p else jnp.where(odd, update_other, update)
            fresh = weight() - 0.02 * chosen
            copy[p] = fresh.astype(jnp.bfloat16)
            if k == 0:
                (new_out if p else new_in)[...] = fresh
                (up_out if p else up_in)[...] = chosen
    for k, pair in enumerate((firsts, seconds)):
        pair[0][...] = jnp.where(odd, back[k], news[k])
        pair[1][...] = jnp.where(odd, news[k], back[k])


def place_body(numbers, *refs):
    blocks, (copy_in, copy_out, sems) = refs[: len(numbers)], refs[-3:]
    copies = []
    for k, (d, block) in enumerate(zip(numbers, blocks, strict=True)):
        for p, whole in enumerate((copy_in, copy_out)):
            rows = whole.at[slot(d, block.shape[1]), :]
            copies.append(pltpu.make_async_copy(block.at[p], rows, sems.at[2 * k + p]))
    copy_all(copies)


def contract_rows(left, right, precision):
    return lax.dot_general(
        left,
        right,
        (((0,), (0,)), ((), ())),
        precision=precision,
        preferred_element_type=jnp.float32,
    )


def general(
    saved_input,
    cot_inproj,
    cot_outproj,
    factor_inproj,
    factor_outproj,
    weight_inproj,
    weight_outproj,
    first_inproj,
    first_outproj,
    second_inproj,
    second_outproj,
):
    highest = lax.Precision.HIGHEST
    pieces = (
        lax.all_gather(factor_inproj, "fs", axis=0, tiled=True),
        lax.all_gather(factor_outproj, "fs", axis=0, tiled=True),
    )
    mapped_in = jnp.dot(saved_input, pieces[0], preferred_element_type=jnp.float32)
    mapped_out = jnp.dot(saved_input, pieces[1], preferred_element_type=jnp.float32)
    term_in = contract_rows(mapped_in, cot_inproj.astype(jnp.float32), highest)
    term_out = contract_rows(mapped_out, cot_outproj.astype(jnp.float32), highest)
    projected_in, projected_out = (
        lax.psum_scatter(term_in, "fs", scatter_dimension=0, tiled=True),
        lax.psum_scatter(term_out, "fs", scatter_dimension=0, tiled=True),
    )
    first_in_new = 0.8 * first_inproj + 0.2 * projected_in
    first_out_new = 0.8 * first_outproj + 0.2 * projected_out
    second_in_new = 0.9 * second_inproj + 0.1 * projected_in * projected_in
    second_out_new = 0.9 * second_outproj + 0.1 * projected_out * projected_out
    small_in = first_in_new / (jnp.sqrt(second_in_new) + 1e-08)
    small_out = first_out_new / (jnp.sqrt(second_out_new) + 1e-08)
    wide_in = factor_inproj.astype(jnp.float32)
    wide_out = factor_outproj.astype(jnp.float32)
    pieces = (
        lax.all_gather(small_in, "fs", axis=0, tiled=True),
        lax.all_gather(small_out, "fs", axis=0, tiled=True),
    )
    full_in = jnp.dot(wide_in, pieces[0], precision=highest)
    full_out = jnp.dot(wide_out, pieces[1], precision=highest)
    square_in, square_out = lax.psum(
        (jnp.sum(full_in * full_in), jnp.sum(full_out * full_out)), ("fs", "tp")
    )
    entries = float(full_in.shape[0] * full_in.shape[1] * lax.axis_size("fs") * lax.axis_size("tp"))
    update_in = full_in / jnp.sqrt(square_in / entries + 1e-06)
    update_out = full_out / jnp.sqrt(square_out / entries + 1e-06)
    fresh_in = weight_inproj - 0.02 * update_in
    fresh_out = weight_outproj - 0.02 * update_out
    copy_in, copy_out = (
        lax.all_gather(fresh_in.astype(jnp.bfloat16), "fs", axis=0, tiled=True),
        lax.all_gather(fresh_out.astype(jnp.bfloat16), "fs", axis=0, tiled=True),
    )
    return (
        update_in,
        update_out,
        fresh_in,
        fresh_out,
        copy_in,
        copy_out,
        first_in_new,
        first_out_new,
        second_in_new,
        second_out_new,
    )


def pairwise(
    saved_input,
    cot_inproj,
    cot_outproj,
    factor_inproj,
    factor_outproj,
    weight_inproj,
    weight_outproj,
    first_inproj,
    first_outproj,
    second_inproj,
    second_outproj,
):
    size, split = lax.axis_size("fs"), lax.axis_size("tp")
    f32 = functools.partial(jax.ShapeDtypeStruct, dtype=jnp.float32)
    depth, rank = factor_inproj.shape
    tokens, columns = cot_inproj.shape
    rows = rank // size
    like = jax.ShapeDtypeStruct
    dma = pltpu.SemaphoreType.DMA

    factor = call(
        pick_body,
        like((depth, rank), factor_inproj.dtype),
        factor_inproj,
        factor_outproj,
        scratch=[dma],
        hbm=range(2),
        flops=depth * rank,
    )
    f4 = send(factor, "fs", 4)
    f2 = send(factor, "fs", 2)
    f1 = send(factor, "fs", 1)
    half = depth // 2

    def picked(c0, c1, f0, f1, s0, s1, g0, g1, w0, w1, *rest):
        picked_body((c0, c1), (f0, f1), (s0, s1), (g0, g1), (w0, w1), *rest)

    cot_theirs, moments_theirs, factor_theirs, both, early4, late4 = call(
        picked,
        (
            like((tokens, columns), cot_inproj.dtype),
            f32((2, rows, columns)),
            like((depth, rank), factor_inproj.dtype),
            f32((2, depth, columns)),
            f32((2 * depth - half, columns)),
            f32((half, columns)),
        ),
        *(cot_inproj, cot_outproj, first_inproj, first_outproj, second_inproj, second_outproj),
        *(factor_inproj, factor_outproj, weight_inproj, weight_outproj),
        scratch=[dma((9,))],
        hbm=range(10),
        flops=tokens * columns,
    )
    cot_peer = send(cot_theirs, "tp", 1)
    f3 = send(f2, "fs", 1)
    f6 = send(f4, "fs", 2)
    w4a = send(early4, "fs", 4)
    f5 = send(f4, "fs", 1)
    f7 = send(f6, "fs", 1)
    w2in = send(weight_inproj, "fs", 2)
    w2out = send(weight_outproj, "fs", 2)
    early, late = (0, 1, 2, 4), (3, 5, 6, 7)
    factors = (factor, f1, f2, f3, f4, f5, f6, f7)
    mapped = call(
        functools.partial(map_body, early),
        f32((tokens, rank)),
        saved_input,
        *(factors[k] for k in early),
        scratch=[pltpu.VMEM((len(early), tokens, depth), saved_input.dtype), dma((len(early),))],
        hbm=(0,),
        flops=2 * tokens * rank * depth * len(early),
    )
    pair = f32((2, rows, 2 * columns))
    far, near, own = call(
        functools.partial(term_body, size, late),
        (pair, pair, f32((size, rows, 2 * columns))),
        saved_input,
        mapped,
        *(factors[k] for k in late),
        cot_inproj,
        cot_outproj,
        cot_peer,
        scratch=[
            pltpu.VMEM((len(late), tokens, depth), saved_input.dtype),
            pltpu.VMEM((tokens, columns), cot_inproj.dtype),
            dma((len(late),)),
            dma,
        ],
        hbm=(0, 2 + len(late), 3 + len(late)),
        flops=2 * tokens * rank * (depth * len(late) + 6 * columns),
    )
    square = call(
        functools.partial(square_body, size),
        f32((rank, rank)),
        *factors,
        scratch=[pltpu.VMEM((depth * size, rank), factor.dtype)],
        flops=2 * rank * rank * depth * size,
    )

    rfar = send(far, "fs", 1)
    rnear = send(near, "fs", 1)
    w1 = send(both, "fs", 1)
    block = f32((rows, 2 * columns))
    a4, a6 = call(add_body, (block, block), own, rfar, flops=2 * rows * columns)
    a2 = call(add_near_body, block, own, rnear, flops=rows * columns)
    r4 = send(a4, "fs", 4)
    r6 = send(a6, "fs", 6)
    r2 = send(a2, "fs", 2)
    peer = send(moments_theirs, "tp", 1)
    g1, g2, g4 = send(f1, "tp", 1), send(f2, "tp", 1), send(f4, "tp", 1)
    halves = f32((2, rows, columns))
    small, news, others_news = call(
        moments_body,
        (block, halves, halves),
        *(own, rnear, r4, r6, r2),
        *(first_inproj, first_outproj, second_inproj, second_outproj, peer),
        flops=30 * rows * columns,
    )

    s4 = send(small, "fs", 4)
    s2 = send(small, "fs", 2)
    s1 = send(small, "fs", 1)
    s6 = send(s4, "fs", 2)
    s3 = send(s2, "fs", 1)
    s5 = send(s4, "fs", 1)
    s7 = send(s6, "fs", 1)
    w4b = send(late4, "fs", 4)
    back = send(others_news, "tp", 1)
    total, small_mine, small_other = call(
        functools.partial(sum_body, size),
        (f32((8, 128)), f32((rank, columns)), f32((rank, columns))),
        square,
        *(small, s1, s2, s3, s4, s5, s6, s7),
        flops=2 * rank * 2 * columns * 6 * rank,
    )
    sums = [total] + [send(total, "tp", k) for k in (2, 3, 1)]
    small_other = send(small_other, "tp", 1)
    fours, flops = f32((4, depth, columns)), 2 * rank * columns * 12 * depth
    full = call(full_body, fours, small_mine, *(factor, f1, f2, f4), flops=flops)
    full_other = call(full_body, fours, small_other, *(factor_theirs, g1, g2, g4), flops=flops)
    entries = float(depth * size * columns * split)

    def finish(t, n2, n3, n1, full_ref, other_ref, w_in, w_out, w1, w2in, w2out, w4a, w4b, *refs):
        weights = (
            (lambda: w_in[...], lambda: w_out[...]),
            (lambda: w1[0], lambda: w1[1]),
            (lambda: w2in[...], lambda: w2out[...]),
            (
                lambda: w4a[:depth, :],
                lambda: jnp.concatenate([w4a[depth:, :], w4b[...]], axis=0),
            ),
        )
        news_ref, back_ref, *refs = refs
        outs = (*refs[:4], refs[4:8], refs[8:10], refs[10:12])
        sums = (t, n2, n1, n3)
        finish_body(entries, sums, full_ref, other_ref, weights, news_ref, back_ref, outs)

    shard, copy = f32((depth, columns)), like((2, depth, columns), jnp.bfloat16)
    outs = call(
        finish,
        (shard,) * 4 + (copy,) * 4 + (f32((rows, columns)),) * 4,
        *sums,
        full,
        full_other,
        *(weight_inproj, weight_outproj, w1, w2in, w2out, w4a, w4b, news, back),
        flops=40 * depth * columns,
    )
    c0, c1, c2, c4 = outs[4:8]
    c6 = send(c4, "fs", 2)
    c5 = send(c4, "fs", 1)
    c7 = send(c6, "fs", 1)
    c3 = send(c1, "fs", 2)
    whole = like((depth * size, columns), jnp.bfloat16)
    copies = (whole, whole)
    for numbers, blocks in (((0, 1, 2, 4, 5, 6), (c0, c1, c2, c4, c5, c6)), ((3, 7), (c3, c7))):
        count = len(numbers)
        first = copies[0] is whole
        copies = call(
            functools.partial(place_body, numbers),
            (whole, whole),
            *blocks,
            *(() if first else copies),
            scratch=[dma((2 * count,))],
            hbm=() if first else (count, count + 1),
            out=HBM,
            aliases={} if first else {count: 0, count + 1: 1},
            flops=depth * columns,
        )
    return (*outs[:4], *copies, *outs[8:])


def layer(*args):
    return pairwise(*args)


def solution(mesh):
    rows, split = P("fs", None), P("fs", "tp")
    paired = mesh.shape["fs"] == 8 and mesh.shape["tp"] == 4
    return jax.shard_map(
        layer if paired else general,
        mesh=mesh,
        in_specs=(rows, split, split, rows, rows) + (split,) * 6,
        out_specs=(split,) * 4 + (P(None, "tp"),) * 2 + (split,) * 4,
        check_vma=False,
    )
```

```python
import functools

import jax
import jax.numpy as jnp
from jax import lax
from jax.experimental import pallas as pl
from jax.experimental.pallas import tpu as pltpu
from jax.sharding import PartitionSpec as P

HIGHEST = lax.Precision.HIGHEST
VMEM = pl.BlockSpec(memory_space=pltpu.VMEM)
HBM = pl.BlockSpec(memory_space=pltpu.HBM)
VMEM_BYTES = 16 * 2**20
ROWS = (((0,), (0,)), ((), ()))


def send(x, axis, bit):
    size = lax.axis_size(axis)
    return lax.ppermute(x, axis, [(i, i ^ bit) for i in range(size)])


def thirds(x):
    high = x.astype(jnp.bfloat16)
    rest = x - high.astype(jnp.float32)
    middle = rest.astype(jnp.bfloat16)
    low = (rest - middle.astype(jnp.float32)).astype(jnp.bfloat16)
    return high, middle, low


def exact_dot(left, right, dims=(((1,), (0,)), ((), ()))):
    wide = left.dtype == jnp.float32
    total = None
    for part in thirds(left if wide else right)[::-1]:
        pair = (part, right) if wide else (left, part)
        term = lax.dot_general(*pair, dims, preferred_element_type=jnp.float32)
        total = term if total is None else total + term
    return total


def call(body, outs, *args, scratch=(), flops, hbm=(), out=VMEM, aliases={}):
    size = sum(a.size * a.dtype.itemsize for a in args)
    args = [
        pltpu.with_memory_space_constraint(a, pltpu.HBM) if k in hbm else a
        for k, a in enumerate(args)
    ]
    return pl.pallas_call(
        body,
        out_shape=outs,
        in_specs=[HBM if k in hbm else VMEM for k in range(len(args))],
        out_specs=jax.tree.map(lambda _: out, outs),
        scratch_shapes=list(scratch),
        input_output_aliases=aliases,
        compiler_params=pltpu.CompilerParams(vmem_limit_bytes=VMEM_BYTES),
        cost_estimate=pl.CostEstimate(flops=flops, bytes_accessed=size, transcendentals=0),
    )(*args)


def is_odd():
    return lax.axis_index("tp") % 2 == 1


def slot(d, rows):
    return pl.ds(pl.multiple_of((lax.axis_index("fs") ^ d) * rows, rows), rows)


def copy_all(copies):
    for copy in copies:
        copy.start()
    for copy in copies:
        copy.wait()


def pick_body(even, odd, out, sem):
    @pl.when(is_odd())
    def _():
        copy_all([pltpu.make_async_copy(odd, out, sem)])

    @pl.when(jnp.logical_not(is_odd()))
    def _():
        copy_all([pltpu.make_async_copy(even, out, sem)])


def picked_body(saved, cots, firsts, seconds, factors, weights, outs, sems):
    held, own, cot, moments, factor, both = outs

    def copies(k):
        pairs = (
            (cots[k], cot),
            (cots[1 - k], own),
            (saved, held),
            (firsts[k], moments.at[0]),
            (seconds[k], moments.at[1]),
            (factors[k], factor),
            (weights[0], both.at[0]),
            (weights[1], both.at[1]),
        )
        return [pltpu.make_async_copy(*pair, sems.at[i]) for i, pair in enumerate(pairs)]

    @pl.when(is_odd())
    def _():
        copy_all(copies(0))

    @pl.when(jnp.logical_not(is_odd()))
    def _():
        copy_all(copies(1))


def add_blocks(total, saved_ref, factors, numbers):
    for d, factor in zip(numbers, factors, strict=True):
        total = total + jnp.dot(
            saved_ref[:, slot(d, factor.shape[0])], factor[...], preferred_element_type=jnp.float32
        )
    return total


def map_body(numbers, saved_ref, *refs):
    mapped = jnp.zeros(refs[-1].shape, jnp.float32)
    refs[-1][...] = add_blocks(mapped, saved_ref, refs[:-1], numbers)


def term_body(size, numbers, saved_ref, mapped_ref, *refs):
    cot, peer, far, near, own = refs[len(numbers) :]
    mapped = add_blocks(mapped_ref[...], saved_ref, refs[: len(numbers)], numbers)
    columns = cot.shape[1]
    rows = mapped.shape[1] // size
    here = lax.axis_index("fs")
    for side, right in enumerate((cot, peer)):
        term = exact_dot(mapped, right[...], ROWS)
        at = slice(side * columns, (side + 1) * columns)
        for k in range(size):
            own[here ^ k, :, at] = term[k * rows : (k + 1) * rows, :]
    for ref, first in ((far, 7), (near, 3)):
        ref[0] = own[first]
        ref[1] = own[first - 2]


def add_body(own, far, a4, a6):
    a4[...] = own[4] + far[1]
    a6[...] = own[6] + far[0]


def add_near_body(own, near, a2):
    a2[...] = own[2] + near[0]


def moments_body(own, near, r4, r6, r2, f_in, f_out, s_in, s_out, peer, small, mine, other):
    odd = is_odd()
    projected = own[0] + near[1] + r4[...] + r6[...] + r2[...]
    columns = f_in.shape[1]
    pairs = (
        (jnp.where(odd, f_out[...], f_in[...]), jnp.where(odd, s_out[...], s_in[...]), mine),
        (peer[0], peer[1], other),
    )
    for side, (first, second, new) in enumerate(pairs):
        at = slice(side * columns, (side + 1) * columns)
        x = projected[:, at]
        first_new = 0.8 * first + 0.2 * x
        second_new = 0.9 * second + 0.1 * x * x
        new[0] = first_new
        new[1] = second_new
        small[:, at] = first_new / (jnp.sqrt(second_new) + 1e-08)


def square_body(size, *refs):
    factors, (square_ref, held) = refs[:size], refs[size:]
    for d, factor in enumerate(factors):
        held[slot(d, factor.shape[0]), :] = factor[...]
    square_ref[...] = lax.dot_general(
        held[...], held[...], ROWS, preferred_element_type=jnp.float32
    )


def sum_body(size, square_ref, *refs):
    smalls, (sum_ref, mine_ref, other_ref) = refs[:size], refs[size:]
    columns = mine_ref.shape[1]
    for d, small in enumerate(smalls):
        at = slot(d, small.shape[0])
        mine_ref[at, :] = small[:, :columns]
        other_ref[at, :] = small[:, columns:]
    product = sum(
        ref[...] * jnp.dot(square_ref[...], ref[...], precision=HIGHEST)
        for ref in (mine_ref, other_ref)
    )
    sum_ref[...] = jnp.full(sum_ref.shape, jnp.sum(product), jnp.float32)


def full_body(small_ref, *refs):
    small, full_ref = thirds(small_ref[...])[::-1], refs[-1]
    for k, factor in enumerate(refs[:-1]):
        full_ref[k] = sum(
            jnp.dot(factor[...], part, preferred_element_type=jnp.float32) for part in small
        )


def scales(entries, sums):
    t, n2, n3, n1 = sums
    for pair in ((t, n2), (n1, n3)):
        mean = jnp.maximum(pair[0][...] + pair[1][...], 0.0) / entries
        yield (1.0 / jnp.sqrt(mean + 1e-06))[0:1, 0:1]


def updates(k, scaled, full_ref, other_ref):
    odd = is_odd()
    mine, other = full_ref[k] * scaled[0], other_ref[k] * scaled[1]
    return jnp.where(odd, other, mine), jnp.where(odd, mine, other)


def ahead_body(entries, *refs):
    full_ref, other_ref, *weights, both, c_in, c_out = refs[4:]
    chosen = updates(3, tuple(scales(entries, refs[:4])), full_ref, other_ref)
    for p, copy in enumerate((c_in, c_out)):
        copy[...] = (weights[p][...] - 0.02 * chosen[p]).astype(jnp.bfloat16)
        both[p] = copy[...]


def finish_body(entries, *refs):
    full_ref, other_ref, w_in, w_out, w1, w2in, w2out, news, back = refs[4:13]
    ups, fresh, copies, firsts, seconds = (
        refs[13:15],
        refs[15:17],
        refs[17:20],
        refs[20:22],
        refs[22:24],
    )
    scaled = tuple(scales(entries, refs[:4]))
    weights = ((w_in, w_out), (w1.at[0], w1.at[1]), (w2in, w2out))
    for k, (copy, pair) in enumerate(zip(copies, weights, strict=True)):
        for p, chosen in enumerate(updates(k, scaled, full_ref, other_ref)):
            new = pair[p][...] - 0.02 * chosen
            copy[p] = new.astype(jnp.bfloat16)
            if k == 0:
                fresh[p][...] = new
                ups[p][...] = chosen
    odd = is_odd()
    for k, pair in enumerate((firsts, seconds)):
        pair[0][...] = jnp.where(odd, back[k], news[k])
        pair[1][...] = jnp.where(odd, news[k], back[k])


def place_body(pieces, *refs):
    blocks, (*whole, sems) = refs[: len(pieces)], refs[-3:]
    copies = []
    for (d, only), block in zip(pieces, blocks, strict=True):
        for p in (0, 1) if only is None else (only,):
            rows = whole[p].at[slot(d, block.shape[-2]), :]
            source = block.at[p] if only is None else block
            copies.append(pltpu.make_async_copy(source, rows, sems.at[len(copies)]))
    copy_all(copies)


def contract_rows(left, right, precision):
    return lax.dot_general(
        left,
        right,
        (((0,), (0,)), ((), ())),
        precision=precision,
        preferred_element_type=jnp.float32,
    )


def general(
    saved_input,
    cot_inproj,
    cot_outproj,
    factor_inproj,
    factor_outproj,
    weight_inproj,
    weight_outproj,
    first_inproj,
    first_outproj,
    second_inproj,
    second_outproj,
):
    highest = lax.Precision.HIGHEST
    pieces = (
        lax.all_gather(factor_inproj, "fs", axis=0, tiled=True),
        lax.all_gather(factor_outproj, "fs", axis=0, tiled=True),
    )
    mapped_in = jnp.dot(saved_input, pieces[0], preferred_element_type=jnp.float32)
    mapped_out = jnp.dot(saved_input, pieces[1], preferred_element_type=jnp.float32)
    term_in = contract_rows(mapped_in, cot_inproj.astype(jnp.float32), highest)
    term_out = contract_rows(mapped_out, cot_outproj.astype(jnp.float32), highest)
    projected_in, projected_out = (
        lax.psum_scatter(term_in, "fs", scatter_dimension=0, tiled=True),
        lax.psum_scatter(term_out, "fs", scatter_dimension=0, tiled=True),
    )
    first_in_new = 0.8 * first_inproj + 0.2 * projected_in
    first_out_new = 0.8 * first_outproj + 0.2 * projected_out
    second_in_new = 0.9 * second_inproj + 0.1 * projected_in * projected_in
    second_out_new = 0.9 * second_outproj + 0.1 * projected_out * projected_out
    small_in = first_in_new / (jnp.sqrt(second_in_new) + 1e-08)
    small_out = first_out_new / (jnp.sqrt(second_out_new) + 1e-08)
    wide_in = factor_inproj.astype(jnp.float32)
    wide_out = factor_outproj.astype(jnp.float32)
    pieces = (
        lax.all_gather(small_in, "fs", axis=0, tiled=True),
        lax.all_gather(small_out, "fs", axis=0, tiled=True),
    )
    full_in = jnp.dot(wide_in, pieces[0], precision=highest)
    full_out = jnp.dot(wide_out, pieces[1], precision=highest)
    square_in, square_out = lax.psum(
        (jnp.sum(full_in * full_in), jnp.sum(full_out * full_out)), ("fs", "tp")
    )
    entries = float(full_in.shape[0] * full_in.shape[1] * lax.axis_size("fs") * lax.axis_size("tp"))
    update_in = full_in / jnp.sqrt(square_in / entries + 1e-06)
    update_out = full_out / jnp.sqrt(square_out / entries + 1e-06)
    fresh_in = weight_inproj - 0.02 * update_in
    fresh_out = weight_outproj - 0.02 * update_out
    copy_in, copy_out = (
        lax.all_gather(fresh_in.astype(jnp.bfloat16), "fs", axis=0, tiled=True),
        lax.all_gather(fresh_out.astype(jnp.bfloat16), "fs", axis=0, tiled=True),
    )
    return (
        update_in,
        update_out,
        fresh_in,
        fresh_out,
        copy_in,
        copy_out,
        first_in_new,
        first_out_new,
        second_in_new,
        second_out_new,
    )


def pairwise(
    saved_input,
    cot_inproj,
    cot_outproj,
    factor_inproj,
    factor_outproj,
    weight_inproj,
    weight_outproj,
    first_inproj,
    first_outproj,
    second_inproj,
    second_outproj,
):
    size, split = lax.axis_size("fs"), lax.axis_size("tp")
    f32 = functools.partial(jax.ShapeDtypeStruct, dtype=jnp.float32)
    depth, rank = factor_inproj.shape
    tokens, columns = cot_inproj.shape
    rows = rank // size
    like = jax.ShapeDtypeStruct
    dma = pltpu.SemaphoreType.DMA

    factor = call(
        pick_body,
        like((depth, rank), factor_inproj.dtype),
        factor_inproj,
        factor_outproj,
        scratch=[dma],
        hbm=range(2),
        flops=depth * rank,
    )
    f4 = send(factor, "fs", 4)
    f2 = send(factor, "fs", 2)
    f1 = send(factor, "fs", 1)

    def picked(saved, c0, c1, f0, f1, s0, s1, g0, g1, w0, w1, *rest):
        outs, sems = rest[:-1], rest[-1]
        picked_body(saved, (c0, c1), (f0, f1), (s0, s1), (g0, g1), (w0, w1), outs, sems)

    saved, cot, cot_theirs, moments_theirs, factor_theirs, both = call(
        picked,
        (
            like(saved_input.shape, saved_input.dtype),
            like((tokens, columns), cot_inproj.dtype),
            like((tokens, columns), cot_inproj.dtype),
            f32((2, rows, columns)),
            like((depth, rank), factor_inproj.dtype),
            f32((2, depth, columns)),
        ),
        *(saved_input, cot_inproj, cot_outproj),
        *(first_inproj, first_outproj, second_inproj, second_outproj),
        *(factor_inproj, factor_outproj, weight_inproj, weight_outproj),
        scratch=[dma((8,))],
        hbm=range(11),
        flops=tokens * columns,
    )
    cot_peer = send(cot_theirs, "tp", 1)
    f3 = send(f1, "fs", 2)
    f6 = send(f4, "fs", 2)
    w4in = send(weight_inproj, "fs", 4)
    f5 = send(f4, "fs", 1)
    f7 = send(f6, "fs", 1)
    w2in = send(weight_inproj, "fs", 2)
    w2out = send(weight_outproj, "fs", 2)
    early, late = (0, 1, 2, 4), (3, 5, 6, 7)
    factors = (factor, f1, f2, f3, f4, f5, f6, f7)
    mapped = call(
        functools.partial(map_body, early),
        f32((tokens, rank)),
        saved,
        *(factors[k] for k in early),
        flops=2 * tokens * rank * depth * len(early),
    )
    pair = f32((2, rows, 2 * columns))
    far, near, own = call(
        functools.partial(term_body, size, late),
        (pair, pair, f32((size, rows, 2 * columns))),
        saved,
        mapped,
        *(factors[k] for k in late),
        cot,
        cot_peer,
        flops=2 * tokens * rank * (depth * len(late) + 6 * columns),
    )
    square = call(
        functools.partial(square_body, size),
        f32((rank, rank)),
        *factors,
        scratch=[pltpu.VMEM((depth * size, rank), factor.dtype)],
        flops=2 * rank * rank * depth * size,
    )

    rfar = send(far, "fs", 1)
    rnear = send(near, "fs", 1)
    w1 = send(both, "fs", 1)
    block = f32((rows, 2 * columns))
    a4, a6 = call(add_body, (block, block), own, rfar, flops=2 * rows * columns)
    a2 = call(add_near_body, block, own, rnear, flops=rows * columns)
    r4 = send(a4, "fs", 4)
    r6 = send(a6, "fs", 6)
    r2 = send(a2, "fs", 2)
    peer = send(moments_theirs, "tp", 1)
    g1, g2, g4 = send(f1, "tp", 1), send(f2, "tp", 1), send(f4, "tp", 1)
    halves = f32((2, rows, columns))
    small, news, others_news = call(
        moments_body,
        (block, halves, halves),
        *(own, rnear, r4, r6, r2),
        *(first_inproj, first_outproj, second_inproj, second_outproj, peer),
        flops=30 * rows * columns,
    )

    s4 = send(small, "fs", 4)
    s2 = send(small, "fs", 2)
    s1 = send(small, "fs", 1)
    s6 = send(small, "fs", 6)
    s3 = send(s2, "fs", 1)
    s5 = send(s4, "fs", 1)
    s7 = send(s6, "fs", 1)
    w4out = send(weight_outproj, "fs", 4)
    back = send(others_news, "tp", 1)
    total, small_mine, small_other = call(
        functools.partial(sum_body, size),
        (f32((8, 128)), f32((rank, columns)), f32((rank, columns))),
        square,
        *(small, s1, s2, s3, s4, s5, s6, s7),
        flops=2 * rank * 2 * columns * 6 * rank,
    )
    sums = [total] + [send(total, "tp", k) for k in (2, 3, 1)]
    small_other = send(small_other, "tp", 1)
    fours, flops = f32((4, depth, columns)), 2 * rank * columns * 12 * depth
    full = call(full_body, fours, small_mine, *(factor, f1, f2, f4), flops=flops)
    full_other = call(full_body, fours, small_other, *(factor_theirs, g1, g2, g4), flops=flops)
    entries = float(depth * size * columns * split)
    shard, one = f32((depth, columns)), like((depth, columns), jnp.bfloat16)
    two = like((2, depth, columns), jnp.bfloat16)
    c4, c4in, c4out = call(
        functools.partial(ahead_body, entries),
        (two, one, one),
        *(*sums, full, full_other, w4in, w4out),
        flops=10 * depth * columns,
    )
    c5 = send(c4, "fs", 1)
    c6in, c6out = send(c4in, "fs", 2), send(c4out, "fs", 2)
    outs = call(
        functools.partial(finish_body, entries),
        (shard,) * 4 + (two,) * 3 + (f32((rows, columns)),) * 4,
        *(*sums, full, full_other, weight_inproj, weight_outproj, w1, w2in, w2out, news, back),
        flops=30 * depth * columns,
    )
    c0, c1, c2 = outs[4:7]
    c3 = send(c1, "fs", 2)
    c7in, c7out = send(c6in, "fs", 1), send(c6out, "fs", 1)
    whole = like((depth * size, columns), jnp.bfloat16)
    copies = ()
    for pieces, blocks in (
        (((0, None), (1, None), (2, None), (4, None)), (c0, c1, c2, c4)),
        (((5, None), (6, 0), (6, 1)), (c5, c6in, c6out)),
        (((3, None), (7, 0), (7, 1)), (c3, c7in, c7out)),
    ):
        count = len(pieces)
        copies = call(
            functools.partial(place_body, pieces),
            (whole, whole),
            *blocks,
            *copies,
            scratch=[dma((2 * count,))],
            hbm=range(count, count + len(copies)),
            out=HBM,
            aliases={count + k: k for k in range(len(copies))},
            flops=depth * columns,
        )
    return (*outs[:4], *copies, *outs[7:])


def layer(*args):
    return pairwise(*args)


def solution(mesh):
    rows, split = P("fs", None), P("fs", "tp")
    paired = mesh.shape["fs"] == 8 and mesh.shape["tp"] == 4
    return jax.shard_map(
        layer if paired else general,
        mesh=mesh,
        in_specs=(rows, split, split, rows, rows) + (split,) * 6,
        out_specs=(split,) * 4 + (P(None, "tp"),) * 2 + (split,) * 4,
        check_vma=False,
    )
```

```python
import functools

import jax
import jax.numpy as jnp
from jax import lax
from jax.experimental import pallas as pl
from jax.experimental.pallas import tpu as pltpu
from jax.sharding import PartitionSpec as P

HIGHEST = lax.Precision.HIGHEST
VMEM = pl.BlockSpec(memory_space=pltpu.VMEM)
HBM = pl.BlockSpec(memory_space=pltpu.HBM)
VMEM_BYTES = 16 * 2**20
ROWS = (((0,), (0,)), ((), ()))


def send(x, axis, bit):
    size = lax.axis_size(axis)
    return lax.ppermute(x, axis, [(i, i ^ bit) for i in range(size)])


def thirds(x):
    high = x.astype(jnp.bfloat16)
    rest = x - high.astype(jnp.float32)
    middle = rest.astype(jnp.bfloat16)
    low = (rest - middle.astype(jnp.float32)).astype(jnp.bfloat16)
    return high, middle, low


def exact_dot(left, right, dims=(((1,), (0,)), ((), ()))):
    wide = left.dtype == jnp.float32
    total = None
    for part in thirds(left if wide else right)[::-1]:
        pair = (part, right) if wide else (left, part)
        term = lax.dot_general(*pair, dims, preferred_element_type=jnp.float32)
        total = term if total is None else total + term
    return total


def call(body, outs, *args, scratch=(), flops, hbm=(), out=VMEM, aliases={}):
    size = sum(a.size * a.dtype.itemsize for a in args)
    args = [
        pltpu.with_memory_space_constraint(a, pltpu.HBM) if k in hbm else a
        for k, a in enumerate(args)
    ]
    return pl.pallas_call(
        body,
        out_shape=outs,
        in_specs=[HBM if k in hbm else VMEM for k in range(len(args))],
        out_specs=jax.tree.map(lambda _: out, outs),
        scratch_shapes=list(scratch),
        input_output_aliases=aliases,
        compiler_params=pltpu.CompilerParams(vmem_limit_bytes=VMEM_BYTES),
        cost_estimate=pl.CostEstimate(flops=flops, bytes_accessed=size, transcendentals=0),
    )(*args)


def is_odd():
    return lax.axis_index("tp") % 2 == 1


def slot(d, rows):
    return pl.ds(pl.multiple_of((lax.axis_index("fs") ^ d) * rows, rows), rows)


def copy_all(copies):
    for copy in copies:
        copy.start()
    for copy in copies:
        copy.wait()


def joined(refs, counts):
    at = 0
    for count in counts:
        parts = refs[at : at + count]
        at += count
        if count == 1:
            parts = parts if len(parts[0].shape) == 2 else (parts[0].at[0], parts[0].at[1])
        values = [part[...] for part in parts]
        yield values[0] if len(values) == 1 else jnp.concatenate(values, axis=1)


def pick_body(even, odd, both, left, right, sems):
    width = left.shape[1]

    def copies(source):
        halves = source.at[:, pl.ds(0, width)], source.at[:, pl.ds(width, width)]
        pairs = zip(halves * 2, (left, right, both.at[0], both.at[1]), strict=True)
        return [pltpu.make_async_copy(*pair, sems.at[i]) for i, pair in enumerate(pairs)]

    @pl.when(is_odd())
    def _():
        copy_all(copies(odd))

    @pl.when(jnp.logical_not(is_odd()))
    def _():
        copy_all(copies(even))


def picked_body(saved, cots, firsts, seconds, factors, weights, outs, sems):
    held, own, cot, moments, factor, both = outs

    def copies(k):
        pairs = (
            (cots[k], cot),
            (cots[1 - k], own),
            (saved, held),
            (firsts[k], moments.at[0]),
            (seconds[k], moments.at[1]),
            (factors[k], factor),
            (weights[0], both.at[0]),
            (weights[1], both.at[1]),
        )
        return [pltpu.make_async_copy(*pair, sems.at[i]) for i, pair in enumerate(pairs)]

    @pl.when(is_odd())
    def _():
        copy_all(copies(0))

    @pl.when(jnp.logical_not(is_odd()))
    def _():
        copy_all(copies(1))


def add_blocks(total, saved_ref, refs, counts, numbers):
    for d, factor in zip(numbers, joined(refs, counts), strict=True):
        total = total + jnp.dot(
            saved_ref[:, slot(d, factor.shape[0])], factor, preferred_element_type=jnp.float32
        )
    return total


def map_body(numbers, counts, saved_ref, *refs):
    mapped = jnp.zeros(refs[-1].shape, jnp.float32)
    refs[-1][...] = add_blocks(mapped, saved_ref, refs[:-1], counts, numbers)


def term_body(size, numbers, counts, saved_ref, mapped_ref, *refs):
    cot, peer, far, near, own = refs[sum(counts) :]
    mapped = add_blocks(mapped_ref[...], saved_ref, refs[: sum(counts)], counts, numbers)
    columns = cot.shape[1]
    rows = mapped.shape[1] // size
    here = lax.axis_index("fs")
    for side, right in enumerate((cot, peer)):
        term = exact_dot(mapped, right[...], ROWS)
        at = slice(side * columns, (side + 1) * columns)
        for k in range(size):
            own[here ^ k, :, at] = term[k * rows : (k + 1) * rows, :]
    for ref, first in ((far, 7), (near, 3)):
        ref[0] = own[first]
        ref[1] = own[first - 2]


def add_body(own, far, a4, a6):
    a4[...] = own[4] + far[1]
    a6[...] = own[6] + far[0]


def add_near_body(own, near, a2):
    a2[...] = own[2] + near[0]


def moments_body(own, near, r4, r6, r2, f_in, f_out, s_in, s_out, peer, small, mine, other):
    odd = is_odd()
    projected = own[0] + near[1] + r4[...] + r6[...] + r2[...]
    columns = f_in.shape[1]
    pairs = (
        (jnp.where(odd, f_out[...], f_in[...]), jnp.where(odd, s_out[...], s_in[...]), mine),
        (peer[0], peer[1], other),
    )
    for side, (first, second, new) in enumerate(pairs):
        at = slice(side * columns, (side + 1) * columns)
        x = projected[:, at]
        first_new = 0.8 * first + 0.2 * x
        second_new = 0.9 * second + 0.1 * x * x
        new[0] = first_new
        new[1] = second_new
        small[:, at] = first_new / (jnp.sqrt(second_new) + 1e-08)


def square_body(counts, *refs):
    square_ref, held = refs[sum(counts) :]
    for d, factor in enumerate(joined(refs, counts)):
        held[slot(d, factor.shape[0]), :] = factor
    square_ref[...] = lax.dot_general(
        held[...], held[...], ROWS, preferred_element_type=jnp.float32
    )


def sum_body(size, square_ref, *refs):
    smalls, (sum_ref, mine_ref, other_ref) = refs[:size], refs[size:]
    columns = mine_ref.shape[1]
    for d, small in enumerate(smalls):
        at = slot(d, small.shape[0])
        mine_ref[at, :] = small[:, :columns]
        other_ref[at, :] = small[:, columns:]
    product = sum(
        ref[...] * jnp.dot(square_ref[...], ref[...], precision=HIGHEST)
        for ref in (mine_ref, other_ref)
    )
    sum_ref[...] = jnp.full(sum_ref.shape, jnp.sum(product), jnp.float32)


def full_body(counts, small_ref, *refs):
    small, full_ref = thirds(small_ref[...])[::-1], refs[-1]
    for k, factor in enumerate(joined(refs, counts)):
        full_ref[k] = sum(
            jnp.dot(factor, part, preferred_element_type=jnp.float32) for part in small
        )


def scales(entries, sums):
    t, n2, n3, n1 = sums
    for pair in ((t, n2), (n1, n3)):
        mean = jnp.maximum(pair[0][...] + pair[1][...], 0.0) / entries
        yield (1.0 / jnp.sqrt(mean + 1e-06))[0:1, 0:1]


def updates(k, scaled, full_ref, other_ref):
    odd = is_odd()
    mine, other = full_ref[k] * scaled[0], other_ref[k] * scaled[1]
    return jnp.where(odd, other, mine), jnp.where(odd, mine, other)


def ahead_body(entries, p, *refs):
    full_ref, other_ref, weight, copy = refs[4:]
    chosen = updates(3, tuple(scales(entries, refs[:4])), full_ref, other_ref)[p]
    copy[...] = (weight[...] - 0.02 * chosen).astype(jnp.bfloat16)


def beside_body(entries, *refs):
    full_ref, other_ref, weights, copy = refs[4:]
    for p, chosen in enumerate(updates(1, tuple(scales(entries, refs[:4])), full_ref, other_ref)):
        copy[p] = (weights[p] - 0.02 * chosen).astype(jnp.bfloat16)


def finish_body(entries, *refs):
    full_ref, other_ref, w_in, w_out, w2in, w2out, news, back = refs[4:12]
    ups, fresh, copies, firsts, seconds = (
        refs[12:14],
        refs[14:16],
        refs[16:18],
        refs[18:20],
        refs[20:22],
    )
    scaled = tuple(scales(entries, refs[:4]))
    for k, copy, pair in zip((0, 2), copies, ((w_in, w_out), (w2in, w2out)), strict=True):
        for p, chosen in enumerate(updates(k, scaled, full_ref, other_ref)):
            new = pair[p][...] - 0.02 * chosen
            copy[p] = new.astype(jnp.bfloat16)
            if k == 0:
                fresh[p][...] = new
                ups[p][...] = chosen
    odd = is_odd()
    for k, pair in enumerate((firsts, seconds)):
        pair[0][...] = jnp.where(odd, back[k], news[k])
        pair[1][...] = jnp.where(odd, news[k], back[k])


def place_body(pieces, *refs):
    blocks, (*whole, sems) = refs[: len(pieces)], refs[-3:]
    copies = []
    for (d, only), block in zip(pieces, blocks, strict=True):
        for p in (0, 1) if only is None else (only,):
            rows = whole[p].at[slot(d, block.shape[-2]), :]
            source = block.at[p] if only is None else block
            copies.append(pltpu.make_async_copy(source, rows, sems.at[len(copies)]))
    copy_all(copies)


def contract_rows(left, right, precision):
    return lax.dot_general(
        left,
        right,
        (((0,), (0,)), ((), ())),
        precision=precision,
        preferred_element_type=jnp.float32,
    )


def general(
    saved_input,
    cot_inproj,
    cot_outproj,
    factor_inproj,
    factor_outproj,
    weight_inproj,
    weight_outproj,
    first_inproj,
    first_outproj,
    second_inproj,
    second_outproj,
):
    highest = lax.Precision.HIGHEST
    pieces = (
        lax.all_gather(factor_inproj, "fs", axis=0, tiled=True),
        lax.all_gather(factor_outproj, "fs", axis=0, tiled=True),
    )
    mapped_in = jnp.dot(saved_input, pieces[0], preferred_element_type=jnp.float32)
    mapped_out = jnp.dot(saved_input, pieces[1], preferred_element_type=jnp.float32)
    term_in = contract_rows(mapped_in, cot_inproj.astype(jnp.float32), highest)
    term_out = contract_rows(mapped_out, cot_outproj.astype(jnp.float32), highest)
    projected_in, projected_out = (
        lax.psum_scatter(term_in, "fs", scatter_dimension=0, tiled=True),
        lax.psum_scatter(term_out, "fs", scatter_dimension=0, tiled=True),
    )
    first_in_new = 0.8 * first_inproj + 0.2 * projected_in
    first_out_new = 0.8 * first_outproj + 0.2 * projected_out
    second_in_new = 0.9 * second_inproj + 0.1 * projected_in * projected_in
    second_out_new = 0.9 * second_outproj + 0.1 * projected_out * projected_out
    small_in = first_in_new / (jnp.sqrt(second_in_new) + 1e-08)
    small_out = first_out_new / (jnp.sqrt(second_out_new) + 1e-08)
    wide_in = factor_inproj.astype(jnp.float32)
    wide_out = factor_outproj.astype(jnp.float32)
    pieces = (
        lax.all_gather(small_in, "fs", axis=0, tiled=True),
        lax.all_gather(small_out, "fs", axis=0, tiled=True),
    )
    full_in = jnp.dot(wide_in, pieces[0], precision=highest)
    full_out = jnp.dot(wide_out, pieces[1], precision=highest)
    square_in, square_out = lax.psum(
        (jnp.sum(full_in * full_in), jnp.sum(full_out * full_out)), ("fs", "tp")
    )
    entries = float(full_in.shape[0] * full_in.shape[1] * lax.axis_size("fs") * lax.axis_size("tp"))
    update_in = full_in / jnp.sqrt(square_in / entries + 1e-06)
    update_out = full_out / jnp.sqrt(square_out / entries + 1e-06)
    fresh_in = weight_inproj - 0.02 * update_in
    fresh_out = weight_outproj - 0.02 * update_out
    copy_in, copy_out = (
        lax.all_gather(fresh_in.astype(jnp.bfloat16), "fs", axis=0, tiled=True),
        lax.all_gather(fresh_out.astype(jnp.bfloat16), "fs", axis=0, tiled=True),
    )
    return (
        update_in,
        update_out,
        fresh_in,
        fresh_out,
        copy_in,
        copy_out,
        first_in_new,
        first_out_new,
        second_in_new,
        second_out_new,
    )


def pairwise(
    saved_input,
    cot_inproj,
    cot_outproj,
    factor_inproj,
    factor_outproj,
    weight_inproj,
    weight_outproj,
    first_inproj,
    first_outproj,
    second_inproj,
    second_outproj,
):
    size, split = lax.axis_size("fs"), lax.axis_size("tp")
    f32 = functools.partial(jax.ShapeDtypeStruct, dtype=jnp.float32)
    depth, rank = factor_inproj.shape
    tokens, columns = cot_inproj.shape
    rows = rank // size
    like = jax.ShapeDtypeStruct
    dma = pltpu.SemaphoreType.DMA

    factor, left, right = call(
        pick_body,
        (
            like((2, depth, rank // 2), factor_inproj.dtype),
            like((depth, rank // 2), factor_inproj.dtype),
            like((depth, rank // 2), factor_inproj.dtype),
        ),
        factor_inproj,
        factor_outproj,
        scratch=[dma((4,))],
        hbm=range(2),
        flops=depth * rank,
    )

    def halves(pair, axis, bit):
        return tuple(send(half, axis, bit) for half in pair)

    f4 = halves((left, right), "fs", 4)
    f2 = send(factor, "fs", 2)
    f1 = send(factor, "fs", 1)

    def picked(saved, c0, c1, f0, f1, s0, s1, g0, g1, w0, w1, *rest):
        outs, sems = rest[:-1], rest[-1]
        picked_body(saved, (c0, c1), (f0, f1), (s0, s1), (g0, g1), (w0, w1), outs, sems)

    saved, cot, cot_theirs, moments_theirs, factor_theirs, both = call(
        picked,
        (
            like(saved_input.shape, saved_input.dtype),
            like((tokens, columns), cot_inproj.dtype),
            like((tokens, columns), cot_inproj.dtype),
            f32((2, rows, columns)),
            like((depth, rank), factor_inproj.dtype),
            f32((2, depth, columns)),
        ),
        *(saved_input, cot_inproj, cot_outproj),
        *(first_inproj, first_outproj, second_inproj, second_outproj),
        *(factor_inproj, factor_outproj, weight_inproj, weight_outproj),
        scratch=[dma((8,))],
        hbm=range(11),
        flops=tokens * columns,
    )
    cot_peer = send(cot_theirs, "tp", 1)
    f3 = send(f1, "fs", 2)
    f6 = halves(f4, "fs", 2)
    w4in = send(weight_inproj, "fs", 4)
    f5 = halves(f4, "fs", 1)
    f7 = halves(f6, "fs", 1)
    w2in = send(weight_inproj, "fs", 2)
    w2out = send(weight_outproj, "fs", 2)
    early, late = (0, 1, 2, 4), (3, 5, 6, 7)
    factors = ((factor,), (f1,), (f2,), (f3,), f4, f5, f6, f7)

    def chosen(numbers):
        return tuple(len(factors[k]) for k in numbers), [x for k in numbers for x in factors[k]]

    counts, arrays = chosen(early)
    mapped = call(
        functools.partial(map_body, early, counts),
        f32((tokens, rank)),
        saved,
        *arrays,
        flops=2 * tokens * rank * depth * len(early),
    )
    pair = f32((2, rows, 2 * columns))
    counts, arrays = chosen(late)
    far, near, own = call(
        functools.partial(term_body, size, late, counts),
        (pair, pair, f32((size, rows, 2 * columns))),
        saved,
        mapped,
        *arrays,
        cot,
        cot_peer,
        flops=2 * tokens * rank * (depth * len(late) + 6 * columns),
    )
    counts, arrays = chosen(range(size))
    square = call(
        functools.partial(square_body, counts),
        f32((rank, rank)),
        *arrays,
        scratch=[pltpu.VMEM((depth * size, rank), factor.dtype)],
        flops=2 * rank * rank * depth * size,
    )

    rfar = send(far, "fs", 1)
    rnear = send(near, "fs", 1)
    w1 = send(both, "fs", 1)
    block = f32((rows, 2 * columns))
    a4, a6 = call(add_body, (block, block), own, rfar, flops=2 * rows * columns)
    a2 = call(add_near_body, block, own, rnear, flops=rows * columns)
    r4 = send(a4, "fs", 4)
    r6 = send(a6, "fs", 6)
    r2 = send(a2, "fs", 2)
    peer = send(moments_theirs, "tp", 1)
    g1, g2, g4 = send(f1, "tp", 1), send(f2, "tp", 1), halves(f4, "tp", 1)
    two = f32((2, rows, columns))
    small, news, others_news = call(
        moments_body,
        (block, two, two),
        *(own, rnear, r4, r6, r2),
        *(first_inproj, first_outproj, second_inproj, second_outproj, peer),
        flops=30 * rows * columns,
    )

    s4 = send(small, "fs", 4)
    s2 = send(small, "fs", 2)
    s1 = send(small, "fs", 1)
    s6 = send(small, "fs", 6)
    s3 = send(s2, "fs", 1)
    s5 = send(s4, "fs", 1)
    s7 = send(s6, "fs", 1)
    w4out = send(weight_outproj, "fs", 4)
    back = send(others_news, "tp", 1)
    total, small_mine, small_other = call(
        functools.partial(sum_body, size),
        (f32((8, 128)), f32((rank, columns)), f32((rank, columns))),
        square,
        *(small, s1, s2, s3, s4, s5, s6, s7),
        flops=2 * rank * 2 * columns * 6 * rank,
    )
    sums = [total] + [send(total, "tp", k) for k in (2, 3, 1)]
    small_other = send(small_other, "tp", 1)
    fours, flops = f32((4, depth, columns)), 2 * rank * columns * 12 * depth
    body = functools.partial(full_body, (1, 1, 1, 2))
    full = call(body, fours, small_mine, *(factor, f1, f2, *f4), flops=flops)
    full_other = call(body, fours, small_other, *(factor_theirs, g1, g2, *g4), flops=flops)
    entries = float(depth * size * columns * split)
    shard, one = f32((depth, columns)), like((depth, columns), jnp.bfloat16)
    two = like((2, depth, columns), jnp.bfloat16)
    c4 = [
        call(
            functools.partial(ahead_body, entries, p),
            one,
            *(*sums, full, full_other, weight),
            flops=5 * depth * columns,
        )
        for p, weight in enumerate((w4in, w4out))
    ]
    c6in, c6out = send(c4[0], "fs", 2), send(c4[1], "fs", 2)
    c5in, c5out = send(c4[0], "fs", 1), send(c4[1], "fs", 1)
    c1 = call(
        functools.partial(beside_body, entries),
        two,
        *(*sums, full, full_other, w1),
        flops=10 * depth * columns,
    )
    outs = call(
        functools.partial(finish_body, entries),
        (shard,) * 4 + (two,) * 2 + (f32((rows, columns)),) * 4,
        *(*sums, full, full_other, weight_inproj, weight_outproj, w2in, w2out, news, back),
        flops=30 * depth * columns,
    )
    c0, c2 = outs[4:6]
    c3 = send(c1, "fs", 2)
    c7in, c7out = send(c6in, "fs", 1), send(c6out, "fs", 1)
    whole = like((depth * size, columns), jnp.bfloat16)
    copies = ()
    for pieces, blocks in (
        (((0, None), (1, None), (2, None), (4, 0), (4, 1)), (c0, c1, c2, *c4)),
        (((5, 0), (5, 1), (6, 0), (6, 1)), (c5in, c5out, c6in, c6out)),
        (((3, None), (7, 0), (7, 1)), (c3, c7in, c7out)),
    ):
        count = len(pieces)
        copies = call(
            functools.partial(place_body, pieces),
            (whole, whole),
            *blocks,
            *copies,
            scratch=[dma((2 * count,))],
            hbm=range(count, count + len(copies)),
            out=HBM,
            aliases={count + k: k for k in range(len(copies))},
            flops=depth * columns,
        )
    return (*outs[:4], *copies, *outs[6:])


def layer(*args):
    return pairwise(*args)


def solution(mesh):
    rows, split = P("fs", None), P("fs", "tp")
    paired = mesh.shape["fs"] == 8 and mesh.shape["tp"] == 4
    return jax.shard_map(
        layer if paired else general,
        mesh=mesh,
        in_specs=(rows, split, split, rows, rows) + (split,) * 6,
        out_specs=(split,) * 4 + (P(None, "tp"),) * 2 + (split,) * 4,
        check_vma=False,
    )
```
